128 devices in a mesh: ep: 64 (over z, y, x), tp: 2 (over core).
Axes of the slice: x: 4, y: 4, z: 4, core: 2. Of those that a mesh axis runs over, the one named last changes fastest.
Arguments:
- tokens: bfloat16 [16384, 1024], P('ep'), may hold values from -6 to 6
- norm_gain: float32 [1024], replicated, may hold values from 0.1 to 1.9
- routing: int32 [16384, 2], P('ep'), may hold values from 0 to 127, all different within a row; in each aligned block of 256 rows (0 to 255, 256 to 511, ...) at most 4 rows name the same one
- route_weights: float32 [16384, 2], P('ep'), may hold values from 0.1 to 1
- lengths: int32 [4096], P('ep'), may hold values from 1 to 4, 10240 in all
- w_gate: bfloat16 [128, 1024, 3584], P('ep', None, 'tp'), may hold values from -0.1875 to 0.1875
- w_up: bfloat16 [128, 1024, 3584], P('ep', None, 'tp'), may hold values from -0.1875 to 0.1875
- w_down: bfloat16 [128, 3584, 1024], P('ep', 'tp'), may hold values from -0.09375 to 0.09375
Outputs:
- mixed: bfloat16 [16384, 1024], P('ep', 'tp')
The draws below stay inside these ranges and needn't reach their ends.
Inputs may be any that keep to these rules, and one draw needn't show every extreme that they name: `routing`: each row names 2 different experts; at most 4 rows of one device name the same expert, and that many is reached.
All inputs are finite; a program needn't handle non-finite values. No bound on the sum of `lengths` on one device may be relied on, other than what follows from the above.
Results may differ from the reference program's by a relative error of at most 0.009.
Values may be sent and summed in bfloat16 or wider, within the bound.
No kernel may reach another device: no remote copies, remote signals or barrier semaphores. Data moves between devices by JAX's collectives and lax.ppermute only.
A program may use at most 64 MiB of HBM per device.

```python
import math
import jax
import jax.numpy as jnp
import numpy as np
from jax import lax

D = 1024
FFE = 3584
TOPK = 2
SPAN = 4
TOK_DEV = 256
EXPERTS = 128
CAP = 4
SEQS = 4096
TOKENS = 16384
N_TP = 2


def block_scale(rng, shape, shards, least, top_value):
    factor_of, own = 1.0, jax.random.fold_in(rng, 6)
    for dim, shards_of in shards:
        steps = jnp.exp(jax.random.uniform(jax.random.fold_in(own, dim), (shards_of,), jnp.float32, least / len(shards), top_value / len(shards)))
        factor_of = factor_of * jnp.repeat(steps, shape[dim] // shards_of).reshape([-1 if axis == dim else 1 for axis in range(len(shape))])
    return factor_of


def length_profile(count, total, reach, skew):
    loads = [(1 << 20) // math.isqrt(standing ** skew) + 1 for standing in range(2, count + 1)]
    spare, given = total - reach - (count - 1), [1] * (count - 1)
    while spare > 0:
        candidates = [i for i in range(count - 1) if given[i] < reach]
        whole, remaining = sum([loads[i] for i in candidates]), spare
        for i in candidates:
            more = min(reach - given[i], max(1, remaining * loads[i] // whole), spare)
            given[i] = given[i] + more
            spare = spare - more
    return np.array([reach] + given)


def uneven_parts(stream_key, count, total, most, slope):
    if count == 2:
        one = jax.random.randint(stream_key, (), max(1, total - most), min(most, total - 1) + 1)
        return jnp.stack([one, total - one])
    sizes = jnp.asarray(length_profile(count, total, most, slope), jnp.int32)
    twos = (count - 1) // 2
    giver, receiver = sizes[1:1 + 2 * twos:2], sizes[2:2 + 2 * twos:2]
    room = jnp.minimum(giver - 1, most - receiver)
    passed = jax.random.randint(jax.random.fold_in(stream_key, 1), (twos,), 0, 1 << 20) % (room + 1)
    sizes = sizes.at[1:1 + 2 * twos:2].set(giver - passed).at[2:2 + 2 * twos:2].set(receiver + passed)
    return sizes[jax.random.permutation(jax.random.fold_in(stream_key, 2), count)]


def assign_block(stream_key, own, number, rows, count, top, reach, lean):
    order = jax.random.permutation(stream_key, count)
    heavy_load, ordinary = shares(count, rows * top, reach, lean, True), shares(count, rows * top, reach, lean, False)
    places = jnp.arange(count)

    def named(sizes, rotation):
        used = int((sizes > 0).sum())
        fixed = max(1, used // 4)
        shifted = fixed + (places - fixed + rotation * (used - fixed)) % max(1, count - fixed)
        return jnp.zeros((count,), jnp.int32).at[order[jnp.where(places < fixed, places, shifted)]].set(jnp.asarray(sizes, jnp.int32))

    sizes = jnp.where(number % 4 == 0, named(heavy_load, number // 4), named(ordinary, number - number // 4 - 1))
    mixed = jax.random.permutation(jax.random.fold_in(own, 3), count)
    source_of, sink = mixed[0:count // 2 * 2:2], mixed[1:count // 2 * 2:2]
    margin = jnp.minimum(sizes[source_of] - 1, reach - sizes[sink]) // 2
    margin = jnp.where((source_of == order[0]) | (sink == order[0]) | (sizes[sink] == 0), 0, jnp.maximum(margin, 0))
    shifted = jax.random.randint(jax.random.fold_in(own, 4), (count // 2,), 0, 1 << 20) % (margin + 1)
    sizes = sizes.at[source_of].add(-shifted).at[sink].add(shifted)
    members = jnp.searchsorted(jnp.cumsum(sizes), jnp.arange(rows * top), side="right").astype(jnp.int32)
    table = members.reshape(top, rows).T
    table = table[jax.random.permutation(jax.random.fold_in(own, 1), rows)]
    rotation = jax.random.randint(jax.random.fold_in(own, 2), (rows, 1), 0, top)
    return jnp.take_along_axis(table, (jnp.arange(top)[None, :] + rotation) % top, axis=1)


def shares(count, total, reach, slope, full):
    weights = [(1 << 20) // math.isqrt(grade ** slope) + 1 for grade in range(1, count + 1)]
    largest = reach if full else min(reach, max(-(-total // count), total * weights[0] // sum(weights)))
    least = 1 if total - largest >= count - 1 else 0
    holding, spare = [largest] + [least] * (count - 1), total - largest - least * (count - 1)
    while spare > 0:
        movable = [i for i in range(1, count) if holding[i] < largest] or [i for i in range(1, count) if holding[i] < reach]
        whole, remaining = sum([weights[i] for i in movable]), spare
        for i in movable:
            addition = min(reach - holding[i], max(1, remaining * weights[i] // whole), spare)
            holding[i] = holding[i] + addition
            spare = spare - addition
    return np.array(holding)


def bell_draw(rng, shape, deviation, most, split=(), kind=jnp.bfloat16):
    array = deviation * jax.random.normal(rng, shape, jnp.float32)
    if split:
        array = array * block_scale(rng, shape, split, -0.22, 0.18)
    return jnp.clip(array, -most, most).astype(kind)


def setup_inputs(seed: int = 0) -> dict:
    key_list = jax.random.split(jax.random.key(seed), 9)
    tokens = bell_draw(key_list[0], (TOKENS, D), 1.0, 6.0, ((0, 64),))
    norm_gain = jnp.clip(1.0 + 0.18 * jax.random.normal(key_list[1], (D,), jnp.float32), 0.1, 1.9)
    routing_keys = jax.random.split(jax.random.fold_in(key_list[2], 1), TOKENS // TOK_DEV)
    routing_turns = jax.random.permutation(jax.random.fold_in(key_list[2], 3), TOKENS // TOK_DEV)
    routing = jax.vmap(lambda own, number: assign_block(jax.random.fold_in(key_list[2], 2), own, number, TOK_DEV, EXPERTS, TOPK, CAP, 2))(routing_keys, routing_turns).reshape((TOKENS, TOPK))
    route_weights = jnp.clip(0.1 + 0.9 * jax.random.uniform(key_list[3], (TOKENS, TOPK), jnp.float32) ** block_scale(key_list[3], (TOKENS, TOPK), ((0, 64),), -0.2, 0.2), 0.1, 1.0)
    lengths = uneven_parts(key_list[4], SEQS, SEQS * 5 // 2, SPAN, 2).astype(jnp.int32)
    w_gate = bell_draw(key_list[5], (EXPERTS, D, FFE), D ** -0.5, 0.1875, ((0, 64), (2, 2)))
    w_up = bell_draw(key_list[6], (EXPERTS, D, FFE), D ** -0.5, 0.1875, ((0, 64), (2, 2)))
    w_down = bell_draw(key_list[7], (EXPERTS, FFE, D), FFE ** -0.5, 0.09375, ((0, 64), (1, 2)))
    return {"tokens": tokens, "norm_gain": norm_gain, "routing": routing, "route_weights": route_weights, "lengths": lengths, "w_gate": w_gate, "w_up": w_up, "w_down": w_down}


eps = 1e-06
block_rows = 64

def expert_rows(row_block, gate_mat, up_mat, down_mat):
    gate_proj = jnp.dot(row_block, gate_mat, preferred_element_type=jnp.float32)
    up_proj = jnp.dot(row_block, up_mat, preferred_element_type=jnp.float32)
    hidden = (jax.nn.silu(gate_proj) * up_proj).astype(jnp.bfloat16)
    half_width = FFE // N_TP
    summed = jnp.zeros((row_block.shape[0], D), jnp.float32)
    for core_part in range(N_TP):
        partial_value = jnp.dot(hidden[:, core_part * half_width:(core_part + 1) * half_width], down_mat[core_part * half_width:(core_part + 1) * half_width], preferred_element_type=jnp.float32)
        rounded = lax.optimization_barrier(partial_value.astype(jnp.bfloat16))
        summed = summed + rounded.astype(jnp.float32)
    return summed.astype(jnp.bfloat16)

def reference(tokens, norm_gain, routing, route_weights, lengths, w_gate, w_up, w_down):
    floats = tokens.astype(jnp.float32)
    normed = (floats * lax.rsqrt(lax.optimization_barrier(jnp.mean(floats * floats, axis=-1, keepdims=True)) + eps) * norm_gain).astype(jnp.bfloat16)
    position = jnp.arange(TOKENS, dtype=jnp.int32)
    live_rows = position % SPAN < lengths[position // SPAN]
    flat_ids = jnp.where(live_rows[:, None], routing, EXPERTS).reshape(-1).astype(jnp.int32)
    sorted_picks = jnp.argsort(flat_ids, stable=True).astype(jnp.int32)
    owner_rows = (sorted_picks // TOPK).astype(jnp.int32)
    weight_of = route_weights.reshape(-1)[sorted_picks]
    counts = lax.optimization_barrier(jnp.sum((flat_ids[:, None] == jnp.arange(EXPERTS, dtype=jnp.int32)[None, :]).astype(jnp.int32), axis=0))
    starts = (jnp.cumsum(counts) - counts).astype(jnp.int32)
    total_picks = TOKENS * TOPK

    def expert_step(expert, totals):
        gate_mat = w_gate[expert]
        up_mat = w_up[expert]
        down_mat = w_down[expert]
        first = starts[expert]
        amount = counts[expert]

        def has_more(carry_state):
            return carry_state[0] * block_rows < amount

        def block_step(carry_state):
            block_no, inner = carry_state
            pick_index = first + block_no * block_rows + jnp.arange(block_rows, dtype=jnp.int32)
            in_range = pick_index < first + amount
            clipped = jnp.minimum(pick_index, total_picks - 1).astype(jnp.int32)
            rows_at = owner_rows[clipped]
            result = expert_rows(normed[rows_at], gate_mat, up_mat, down_mat)
            factor = jnp.where(in_range, weight_of[clipped], 0.0)
            inner = inner.at[rows_at].add(factor[:, None] * result.astype(jnp.float32))
            return (block_no + 1, inner)
        ended = lax.while_loop(has_more, block_step, (jnp.int32(0), totals))
        return ended[1]
    totals = lax.fori_loop(0, EXPERTS, expert_step, jnp.zeros((TOKENS, D), jnp.float32))
    return totals.astype(jnp.bfloat16)
```

```python
import jax
import jax.numpy as jnp
from jax import lax
from jax.experimental import pallas as pl
from jax.experimental.pallas import tpu as pltpu
from jax.sharding import PartitionSpec as P

SPAN = 4
SLOTS = 4
CHUNK = 256
eps = 1e-06
f32 = jnp.float32
bf16 = jnp.bfloat16


def dot(a, b):
    return jnp.dot(a, b, preferred_element_type=f32)


def iota(shape, dim):
    return lax.broadcasted_iota(jnp.int32, shape, dim)


def in_hbm(*arrays):
    return [pltpu.with_memory_space_constraint(x, pltpu.HBM) for x in arrays]


def slot_codes(routes, lengths, experts):
    rows = routes.shape[1]
    seqs = lengths.shape[1]
    spread = (iota((seqs, rows), 1) // SPAN == iota((seqs, rows), 0)).astype(bf16)
    spans = dot(jnp.broadcast_to(lengths.astype(bf16), (8, seqs)), spread)[0:1]
    live = (iota((1, rows), 1) % SPAN).astype(f32) < spans
    ids = iota((experts, rows), 0)
    hit = ((routes[0:1] == ids) | (routes[1:2] == ids)) & live
    earlier = (iota((rows, rows), 0) < iota((rows, rows), 1)).astype(bf16)
    before = dot(hit.astype(bf16), earlier)
    return jnp.where(hit, before, -1.0)


def fetch(pairs, sems):
    copies = [pltpu.make_async_copy(src, dst, sems.at[i]) for i, (src, dst) in enumerate(pairs)]
    for copy in copies:
        copy.start()
    return copies


def prep_kernel(
    tok_hbm, gain_hbm, route_hbm, len_hbm, wg_ref, wu_ref, wd_ref,
    out_ref, sg_ref, su_ref, sd_ref,
    tok_ref, gain_ref, route_ref, len_ref, small_sems, sems,
):
    me = lax.axis_index("tp")
    small = fetch(
        ((route_hbm, route_ref), (len_hbm, len_ref), (gain_hbm, gain_ref), (tok_hbm, tok_ref)), small_sems
    )
    copies = [
        pltpu.make_async_copy(w.at[1 - me], s, sems.at[i])
        for i, (w, s) in enumerate(((wg_ref, sg_ref), (wu_ref, su_ref), (wd_ref, sd_ref)))
    ]
    for copy in copies:
        copy.start()
    for copy in small[:2]:
        copy.wait()
    rows, width = tok_ref.shape
    half = width // 2
    slots = out_ref.shape[0]
    chips = slots // 8
    codes = slot_codes(route_ref[...], len_ref[...], 2 * chips).astype(bf16)
    at = iota((slots, 2 * chips), 0)
    mine = (iota((slots, 2 * chips), 1) == 2 * (at // 8) + me).astype(bf16)
    wide = dot(mine, codes)
    row = iota((slots, rows), 0)
    here = wide == (row % SLOTS).astype(f32)
    upper = (row // SLOTS) % 2 == 1
    place_low = jnp.where(here & ~upper, 1.0, 0.0).astype(bf16)
    place_high = jnp.where(here & upper, 1.0, 0.0).astype(bf16)
    for copy in small[2:]:
        copy.wait()
    floats = tok_ref[...].astype(f32)
    scale = lax.rsqrt(jnp.mean(floats * floats, axis=-1, keepdims=True) + eps)
    normed = (floats * scale * gain_ref[...]).astype(bf16)
    out_ref[...] = (dot(place_low, normed[:, :half]) + dot(place_high, normed[:, half:])).astype(bf16)
    for copy in copies:
        copy.wait()


def prep(tokens, gain, routes, lengths, w_gate, w_up, w_down):
    width = tokens.shape[1]
    hidden = w_gate.shape[2]
    chips = lax.axis_size("ep")
    vmem = pl.BlockSpec(memory_space=pltpu.VMEM)
    hbm = pl.BlockSpec(memory_space=pltpu.HBM)
    return pl.pallas_call(
        prep_kernel,
        name="prep",
        out_shape=(
            jax.ShapeDtypeStruct((8 * chips, width // 2), bf16),
            pltpu.VMEM((width, hidden), bf16),
            pltpu.VMEM((width, hidden), bf16),
            pltpu.VMEM((hidden, width), bf16),
        ),
        in_specs=[hbm] * 7,
        out_specs=(vmem,) * 4,
        scratch_shapes=[
            pltpu.VMEM(tokens.shape, bf16),
            pltpu.VMEM(gain.shape, f32),
            pltpu.VMEM(routes.shape, jnp.int32),
            pltpu.VMEM(lengths.shape, jnp.int32),
            pltpu.SemaphoreType.DMA((4,)),
            pltpu.SemaphoreType.DMA((3,)),
        ],
        compiler_params=pltpu.CompilerParams(vmem_limit_bytes=12 << 20),
    )(*in_hbm(tokens, gain, routes, lengths, w_gate, w_up, w_down))


def expert_kernel(in_ref, wg_ref, wu_ref, wd_ref, sg_ref, su_ref, sd_ref, out_ref, g_buf, u_buf, d_buf, x_buf, h_buf, sems):
    me = lax.axis_index("tp")
    width, hidden = g_buf.shape
    half = width // 2
    parts = hidden // CHUNK
    gate_up = []
    for i in range(parts):
        cols = pl.ds(i * CHUNK, CHUNK)
        gate_up.append(
            (
                pltpu.make_async_copy(wg_ref.at[me, :, cols], g_buf.at[:, cols], sems.at[0, i]),
                pltpu.make_async_copy(wu_ref.at[me, :, cols], u_buf.at[:, cols], sems.at[1, i]),
            )
        )
    down = pltpu.make_async_copy(wd_ref.at[me], d_buf, sems.at[2, 0])
    for pair in gate_up:
        for copy in pair:
            copy.start()
    down.start()
    pairs = in_ref.shape[0] // 16
    arrived = in_ref[...].astype(f32).reshape(pairs, 2, 8, half)
    even, odd = arrived[:, 0], arrived[:, 1]
    low = iota((pairs, 8, half), 1) < SLOTS
    first = jnp.where(low, even, pltpu.roll(odd, SLOTS, 1))
    second = jnp.where(low, pltpu.roll(even, SLOTS, 1), odd)
    x_buf[:, :half] = first.reshape(pairs * 8, half).astype(bf16)
    x_buf[:, half:] = second.reshape(pairs * 8, half).astype(bf16)

    def part(gate_ref, up_ref, i, base):
        cols = pl.ds(i * CHUNK, CHUNK)
        x = x_buf[...]
        gate = dot(x, gate_ref[:, cols])
        up = dot(x, up_ref[:, cols])
        h_buf[:, pl.ds(base + i * CHUNK, CHUNK)] = (gate / (1.0 + jnp.exp(-gate)) * up).astype(bf16)

    for i in range(parts):
        part(sg_ref, su_ref, i, 0)
    for i in range(parts):
        for copy in gate_up[i]:
            copy.wait()
        part(g_buf, u_buf, i, hidden)
    down.wait()
    low = iota((pairs, 8, CHUNK), 1) < SLOTS

    def column(i):
        cols = pl.ds(i * CHUNK, CHUNK)
        total = dot(h_buf[:, :hidden], sd_ref[:, cols]) + dot(h_buf[:, hidden:], d_buf[:, cols])
        return total.reshape(pairs, 8, CHUNK)

    for core in range(2):
        a, b = column(2 * core), column(2 * core + 1)
        out_ref[:, 0, core] = jnp.where(low, a, pltpu.roll(b, SLOTS, 1)).astype(bf16)
        out_ref[:, 1, core] = jnp.where(low, pltpu.roll(a, SLOTS, 1), b).astype(bf16)


def expert(arrived, w_gate, w_up, w_down, sg, su, sd):
    width, hidden = sg.shape
    rows = arrived.shape[0] // 2
    vmem = pl.BlockSpec(memory_space=pltpu.VMEM)
    hbm = pl.BlockSpec(memory_space=pltpu.HBM)
    return pl.pallas_call(
        expert_kernel,
        name="expert",
        out_shape=jax.ShapeDtypeStruct((rows // 8, 2, 2, 8, width // 4), bf16),
        in_specs=[vmem] + [hbm] * 3 + [vmem] * 3,
        out_specs=vmem,
        scratch_shapes=[
            pltpu.VMEM((width, hidden), bf16),
            pltpu.VMEM((width, hidden), bf16),
            pltpu.VMEM((hidden, width), bf16),
            pltpu.VMEM((rows, width), bf16),
            pltpu.VMEM((rows, 2 * hidden), bf16),
            pltpu.SemaphoreType.DMA((3, hidden // CHUNK)),
        ],
        compiler_params=pltpu.CompilerParams(vmem_limit_bytes=24 << 20),
    )(arrived, *in_hbm(w_gate, w_up, w_down), sg, su, sd)


def combine_kernel(in_ref, route_ref, len_ref, weight_ref, out_ref):
    slots, quarter = in_ref.shape
    rows = route_ref.shape[1]
    experts = slots // 8
    routes = route_ref[...]
    codes = slot_codes(routes, len_ref[...], experts).astype(bf16)
    ids = iota((experts, rows), 0)
    weights = jnp.where(
        routes[0:1] == ids, weight_ref[0:1], jnp.where(routes[1:2] == ids, weight_ref[1:2], 0.0)
    ).astype(bf16)
    owner = (iota((slots, experts), 0) // 8 == iota((slots, experts), 1)).astype(bf16)
    row = iota((slots, rows), 0)
    picked = jnp.where(dot(owner, codes) == (row % SLOTS).astype(f32), dot(owner, weights), 0.0)
    upper = (row // SLOTS) % 2 == 1
    for part in range(2):
        mix = jnp.where(upper if part else ~upper, picked, 0.0).astype(bf16)
        mixed = lax.dot_general(mix, in_ref[...], (((0,), (0,)), ((), ())), preferred_element_type=f32)
        out_ref[:, part * quarter : (part + 1) * quarter] = mixed.astype(bf16)


def combine(returned, routes, lengths, weights):
    vmem = pl.BlockSpec(memory_space=pltpu.VMEM)
    return pl.pallas_call(
        combine_kernel,
        name="combine",
        out_shape=jax.ShapeDtypeStruct((routes.shape[1], 2 * returned.shape[1]), bf16),
        in_specs=[vmem] * 4,
        out_specs=vmem,
        compiler_params=pltpu.CompilerParams(vmem_limit_bytes=12 << 20),
    )(returned, routes, lengths, weights)


def per_device(tokens, norm_gain, routing, route_weights, lengths, w_gate, w_up, w_down):
    chips = lax.axis_size("ep")
    width = tokens.shape[1]
    routes = routing.T
    weights = route_weights.T
    spans = lengths.reshape(1, -1)
    outgoing, *halves = prep(tokens, norm_gain.reshape(1, -1), routes, spans, w_gate, w_up, w_down)
    swapped = [lax.ppermute(half, "tp", [(0, 1), (1, 0)]) for half in halves]
    arrived = lax.all_to_all(outgoing.reshape(chips, 8, width // 2), "ep", split_axis=0, concat_axis=0, tiled=True)
    results = expert(arrived.reshape(chips * 8, width // 2), w_gate, w_up, w_down, *swapped)
    returned = lax.all_to_all(
        results.reshape(2 * chips, 8, width // 4), ("ep", "tp"), split_axis=0, concat_axis=0, tiled=True
    )
    return combine(returned.reshape(chips * 16, width // 4), routes, spans, weights)


def solution(mesh):
    placed = (
        P("ep", None),
        P(),
        P("ep", None),
        P("ep", None),
        P("ep"),
        P("ep", None, "tp"),
        P("ep", None, "tp"),
        P("ep", "tp", None),
    )
    return jax.shard_map(
        per_device, mesh=mesh, in_specs=placed, out_specs=P("ep", "tp"), check_vma=False
    )
```

```python
import jax
import jax.numpy as jnp
from jax import lax
from jax.experimental import pallas as pl
from jax.experimental.pallas import tpu as pltpu
from jax.sharding import PartitionSpec as P

SPAN = 4
SLOTS = 4
CHUNK = 256
eps = 1e-06
f32 = jnp.float32
bf16 = jnp.bfloat16


def dot(a, b):
    return jnp.dot(a, b, preferred_element_type=f32)


def turned(a, b):
    return lax.dot_general(a, b, (((0,), (0,)), ((), ())), preferred_element_type=f32)


def iota(shape, dim):
    return lax.broadcasted_iota(jnp.int32, shape, dim)


def in_hbm(*arrays):
    return [pltpu.with_memory_space_constraint(x, pltpu.HBM) for x in arrays]


def slot_codes(routes, lengths, experts):
    rows = routes.shape[1]
    seqs = lengths.shape[1]
    spread = (iota((seqs, rows), 1) // SPAN == iota((seqs, rows), 0)).astype(bf16)
    spans = dot(jnp.broadcast_to(lengths.astype(bf16), (8, seqs)), spread)[0:1]
    live = (iota((1, rows), 1) % SPAN).astype(f32) < spans
    ids = iota((experts, rows), 0)
    hit = ((routes[0:1] == ids) | (routes[1:2] == ids)) & live
    earlier = (iota((rows, rows), 0) < iota((rows, rows), 1)).astype(bf16)
    before = dot(hit.astype(bf16), earlier)
    return jnp.where(hit, before, -1.0)


def fetch(pairs, sems):
    copies = [pltpu.make_async_copy(src, dst, sems.at[i]) for i, (src, dst) in enumerate(pairs)]
    for copy in copies:
        copy.start()
    return copies


def prep_kernel(
    tok_hbm, gain_hbm, route_hbm, len_hbm, share_hbm, wg_ref, wu_ref, wd_ref,
    out_ref, mix_ref, sgu_ref, sd_ref,
    tok_ref, gain_ref, route_ref, len_ref, share_ref, small_sems, sems,
):
    me = lax.axis_index("tp")
    small = fetch(
        (
            (route_hbm, route_ref), (len_hbm, len_ref), (tok_hbm, tok_ref), (gain_hbm, gain_ref),
            (share_hbm, share_ref),
        ),
        small_sems,
    )
    large = fetch(
        ((wg_ref.at[1 - me], sgu_ref.at[0]), (wu_ref.at[1 - me], sgu_ref.at[1]), (wd_ref.at[1 - me], sd_ref)), sems
    )
    for copy in small[:2]:
        copy.wait()
    rows, width = tok_ref.shape
    half = width // 2
    slots = out_ref.shape[0]
    experts = slots // 4
    routes = route_ref[...]
    codes = slot_codes(routes, len_ref[...], experts).astype(bf16)
    at = iota((slots, experts), 0)
    mine = (iota((slots, experts), 1) == 2 * (at // 8) + me).astype(bf16)
    wide = dot(mine, codes)
    row = iota((slots, rows), 0)
    here = wide == (row % SLOTS).astype(f32)
    upper = (row // SLOTS) % 2 == 1
    place_low = jnp.where(here & ~upper, 1.0, 0.0).astype(bf16)
    place_high = jnp.where(here & upper, 1.0, 0.0).astype(bf16)
    for copy in small[2:]:
        copy.wait()
    floats = tok_ref[...].astype(f32)
    scale = lax.rsqrt(jnp.mean(floats * floats, axis=-1, keepdims=True) + eps)
    normed = (floats * scale * gain_ref[...]).astype(bf16)
    out_ref[...] = (dot(place_low, normed[:, :half]) + dot(place_high, normed[:, half:])).astype(bf16)
    ids = iota((experts, rows), 0)
    shares = jnp.where(
        routes[0:1] == ids, share_ref[0:1], jnp.where(routes[1:2] == ids, share_ref[1:2], 0.0)
    ).astype(bf16)
    owner = (iota((experts, 2 * slots), 0) == iota((experts, 2 * slots), 1) // 8).astype(bf16)
    column = iota((rows, 2 * slots), 1)
    chosen = turned(codes, owner) == (column % SLOTS).astype(f32)
    picked = jnp.where(chosen, turned(shares, owner), 0.0)
    upper = (column // SLOTS) % 2 == 1
    mix_ref[0] = jnp.where(upper, 0.0, picked).astype(bf16)
    mix_ref[1] = jnp.where(upper, picked, 0.0).astype(bf16)
    for copy in large:
        copy.wait()


def prep(tokens, gain, routes, lengths, shares, w_gate, w_up, w_down):
    rows, width = tokens.shape
    hidden = w_gate.shape[2]
    chips = lax.axis_size("ep")
    return pl.pallas_call(
        prep_kernel,
        name="prep",
        out_shape=(
            jax.ShapeDtypeStruct((8 * chips, width // 2), bf16),
            pltpu.VMEM((2, rows, 16 * chips), bf16),
            pltpu.VMEM((2, width, hidden), bf16),
            pltpu.VMEM((hidden, width), bf16),
        ),
        in_specs=[pl.BlockSpec(memory_space=pltpu.HBM)] * 8,
        out_specs=(pl.BlockSpec(memory_space=pltpu.VMEM),) * 4,
        scratch_shapes=[
            pltpu.VMEM(tokens.shape, bf16),
            pltpu.VMEM(gain.shape, f32),
            pltpu.VMEM(routes.shape, jnp.int32),
            pltpu.VMEM(lengths.shape, jnp.int32),
            pltpu.VMEM(shares.shape, f32),
            pltpu.SemaphoreType.DMA((5,)),
            pltpu.SemaphoreType.DMA((3,)),
        ],
        compiler_params=pltpu.CompilerParams(vmem_limit_bytes=12 << 20),
    )(*in_hbm(tokens, gain, routes, lengths, shares, w_gate, w_up, w_down))


def expert_kernel(
    in_ref, sgu_ref, sd_ref, wg_ref, wu_ref, wd_ref, out_ref,
    gu_buf, d_buf, x_buf, y_buf, h_buf, sum_buf, gu_sems, d_sems,
):
    me = lax.axis_index("tp")
    hidden, width = d_buf.shape
    half = width // 2
    parts = hidden // CHUNK
    blocks = width // CHUNK
    pieces = []
    for i in range(blocks):
        rows = pl.ds(i * CHUNK, CHUNK)
        pieces.append((wg_ref.at[me, rows], gu_buf.at[0, rows]))
        pieces.append((wu_ref.at[me, rows], gu_buf.at[1, rows]))
    gate_up = fetch(pieces, gu_sems)
    pairs = in_ref.shape[0] // 16
    slots = 8 * pairs
    arrived = in_ref[...].astype(f32).reshape(pairs, 2, 8, half)
    even, odd = arrived[:, 0], arrived[:, 1]
    low = iota((pairs, 8, half), 1) < SLOTS
    first = jnp.where(low, even, pltpu.roll(odd, SLOTS, 1)).reshape(slots, half)
    second = jnp.where(low, pltpu.roll(even, SLOTS, 1), odd).reshape(slots, half)
    peak = jnp.zeros((slots, 128), f32)
    for i in range(half // 128):
        lanes = slice(i * 128, (i + 1) * 128)
        peak = jnp.maximum(peak, jnp.maximum(jnp.abs(first[:, lanes]), jnp.abs(second[:, lanes])))
    filled = lax.dot_general(
        jnp.ones((8, 128), bf16), (peak > 0.0).astype(bf16), (((1,), (1,)), ((), ())), preferred_element_type=f32
    )
    live = filled > 0.0
    earlier = (iota((slots, slots), 0) < iota((slots, slots), 1)).astype(bf16)
    place = jnp.where(live, dot(live.astype(bf16), earlier), -1.0)
    amount = jnp.sum(live[0:1].astype(jnp.int32))
    squeeze = (iota((slots, slots), 0).astype(f32) == place[0:1]).astype(bf16)
    x_buf[:, :half] = dot(squeeze, first.astype(bf16)).astype(bf16)
    x_buf[:, half:] = dot(squeeze, second.astype(bf16)).astype(bf16)

    def hide(rows, weights):
        x = x_buf[:rows]
        for i in range(parts):
            cols = pl.ds(i * CHUNK, CHUNK)
            gate = dot(x, weights[0, :, cols])
            up = dot(x, weights[1, :, cols])
            h_buf[:rows, cols] = (gate / (1.0 + jnp.exp(-gate)) * up).astype(bf16)

    def run(rows):
        hide(rows, sgu_ref)
        down = fetch(
            [(wd_ref.at[me, pl.ds(i * CHUNK, CHUNK)], d_buf.at[pl.ds(i * CHUNK, CHUNK)]) for i in range(parts)], d_sems
        )
        for i in range(blocks):
            cols = pl.ds(i * CHUNK, CHUNK)
            sum_buf[:rows, cols] = dot(h_buf[:rows], sd_ref[:, cols])
        for copy in gate_up:
            copy.wait()
        hide(rows, gu_buf)
        for copy in down:
            copy.wait()
        for i in range(blocks):
            cols = pl.ds(i * CHUNK, CHUNK)
            y_buf[:rows, cols] = (sum_buf[:rows, cols] + dot(h_buf[:rows], d_buf[:, cols])).astype(bf16)
        if rows < slots:
            y_buf[rows:] = jnp.zeros((slots - rows, width), bf16)

    few = slots * 3 // 4

    @pl.when(amount <= few)
    def _():
        run(few)

    @pl.when(amount > few)
    def _():
        run(slots)

    low = iota((pairs, 8, CHUNK), 1) < SLOTS

    def spread(i):
        return turned(squeeze, y_buf[:, i * CHUNK : (i + 1) * CHUNK]).reshape(pairs, 8, CHUNK)

    for core in range(2):
        a, b = spread(2 * core), spread(2 * core + 1)
        out_ref[:, 0, core] = jnp.where(low, a, pltpu.roll(b, SLOTS, 1)).astype(bf16)
        out_ref[:, 1, core] = jnp.where(low, pltpu.roll(a, SLOTS, 1), b).astype(bf16)


def expert(arrived, gate_up, down, w_gate, w_up, w_down):
    hidden, width = down.shape
    rows = arrived.shape[0] // 2
    vmem = pl.BlockSpec(memory_space=pltpu.VMEM)
    hbm = pl.BlockSpec(memory_space=pltpu.HBM)
    return pl.pallas_call(
        expert_kernel,
        name="expert",
        out_shape=jax.ShapeDtypeStruct((rows // 8, 2, 2, 8, width // 4), bf16),
        in_specs=[vmem] * 3 + [hbm] * 3,
        out_specs=vmem,
        scratch_shapes=[
            pltpu.VMEM((2, width, hidden), bf16),
            pltpu.VMEM((hidden, width), bf16),
            pltpu.VMEM((rows, width), bf16),
            pltpu.VMEM((rows, width), bf16),
            pltpu.VMEM((rows, hidden), bf16),
            pltpu.VMEM((rows, width), f32),
            pltpu.SemaphoreType.DMA((2 * (width // CHUNK),)),
            pltpu.SemaphoreType.DMA((hidden // CHUNK,)),
        ],
        compiler_params=pltpu.CompilerParams(vmem_limit_bytes=26 << 20),
    )(arrived, gate_up, down, *in_hbm(w_gate, w_up, w_down))


def combine_kernel(in_ref, mix_ref, out_ref):
    quarter = in_ref.shape[1]
    for part in range(2):
        out_ref[:, part * quarter : (part + 1) * quarter] = dot(mix_ref[part], in_ref[...]).astype(bf16)


def combine(returned, mix):
    vmem = pl.BlockSpec(memory_space=pltpu.VMEM)
    return pl.pallas_call(
        combine_kernel,
        name="combine",
        out_shape=jax.ShapeDtypeStruct((mix.shape[1], 2 * returned.shape[1]), bf16),
        in_specs=[vmem] * 2,
        out_specs=vmem,
        compiler_params=pltpu.CompilerParams(vmem_limit_bytes=8 << 20),
    )(returned, mix)


def per_device(tokens, norm_gain, routing, route_weights, lengths, w_gate, w_up, w_down):
    chips = lax.axis_size("ep")
    width = tokens.shape[1]
    routes = routing.T
    weights = route_weights.T
    spans = lengths.reshape(1, -1)
    outgoing, mix, gate_up, down = prep(
        tokens, norm_gain.reshape(1, -1), routes, spans, weights, w_gate, w_up, w_down
    )
    gate_up, down = (lax.ppermute(half, "tp", [(0, 1), (1, 0)]) for half in (gate_up, down))
    arrived = lax.all_to_all(outgoing.reshape(chips, 8, width // 2), "ep", split_axis=0, concat_axis=0, tiled=True)
    results = expert(arrived.reshape(chips * 8, width // 2), gate_up, down, w_gate, w_up, w_down)
    returned = lax.all_to_all(
        results.reshape(2 * chips, 8, width // 4), ("ep", "tp"), split_axis=0, concat_axis=0, tiled=True
    )
    return combine(returned.reshape(chips * 16, width // 4), mix)


def solution(mesh):
    placed = (
        P("ep", None),
        P(),
        P("ep", None),
        P("ep", None),
        P("ep"),
        P("ep", None, "tp"),
        P("ep", None, "tp"),
        P("ep", "tp", None),
    )
    return jax.shard_map(
        per_device, mesh=mesh, in_specs=placed, out_specs=P("ep", "tp"), check_vma=False
    )
```

```python
import jax
import jax.numpy as jnp
from jax import lax
from jax.experimental import pallas as pl
from jax.experimental.pallas import tpu as pltpu
from jax.sharding import PartitionSpec as P

SPAN = 4
SLOTS = 4
CHUNK = 256
eps = 1e-06
f32 = jnp.float32
bf16 = jnp.bfloat16


def dot(a, b):
    return jnp.dot(a, b, preferred_element_type=f32)


def turned(a, b):
    return lax.dot_general(a, b, (((0,), (0,)), ((), ())), preferred_element_type=f32)


def iota(shape, dim):
    return lax.broadcasted_iota(jnp.int32, shape, dim)


def in_hbm(*arrays):
    return [pltpu.with_memory_space_constraint(x, pltpu.HBM) for x in arrays]


def slot_codes(routes, lengths, experts):
    rows = routes.shape[1]
    seqs = lengths.shape[1]
    spread = (iota((seqs, rows), 1) // SPAN == iota((seqs, rows), 0)).astype(bf16)
    spans = dot(jnp.broadcast_to(lengths.astype(bf16), (8, seqs)), spread)[0:1]
    live = (iota((1, rows), 1) % SPAN).astype(f32) < spans
    ids = iota((experts, rows), 0)
    hit = ((routes[0:1] == ids) | (routes[1:2] == ids)) & live
    earlier = (iota((rows, rows), 0) < iota((rows, rows), 1)).astype(bf16)
    before = dot(hit.astype(bf16), earlier)
    return jnp.where(hit, before, -1.0)


def fetch(pairs, sems):
    copies = [pltpu.make_async_copy(src, dst, sems.at[i]) for i, (src, dst) in enumerate(pairs)]
    for copy in copies:
        copy.start()
    return copies


def prep_kernel(
    tok_hbm, gain_hbm, route_hbm, len_hbm, share_hbm, wg_ref, wu_ref, wd_ref,
    out_ref, mix_ref, sgu_ref, sd_ref,
    tok_ref, gain_ref, route_ref, len_ref, share_ref, small_sems, sems,
):
    me = lax.axis_index("tp")
    small = fetch(
        (
            (route_hbm, route_ref), (len_hbm, len_ref), (tok_hbm, tok_ref), (gain_hbm, gain_ref),
            (share_hbm, share_ref),
        ),
        small_sems,
    )
    large = fetch(
        ((wg_ref.at[1 - me], sgu_ref.at[0]), (wu_ref.at[1 - me], sgu_ref.at[1]), (wd_ref.at[1 - me], sd_ref)), sems
    )
    for copy in small[:2]:
        copy.wait()
    rows, width = tok_ref.shape
    half = width // 2
    slots = out_ref.shape[0]
    experts = slots // 4
    routes = route_ref[...]
    codes = slot_codes(routes, len_ref[...], experts).astype(bf16)
    at = iota((slots, experts), 0)
    mine = (iota((slots, experts), 1) == 2 * (at // 8) + me).astype(bf16)
    wide = dot(mine, codes)
    row = iota((slots, rows), 0)
    here = wide == (row % SLOTS).astype(f32)
    upper = (row // SLOTS) % 2 == 1
    place_low = jnp.where(here & ~upper, 1.0, 0.0).astype(bf16)
    place_high = jnp.where(here & upper, 1.0, 0.0).astype(bf16)
    for copy in small[2:]:
        copy.wait()
    floats = tok_ref[...].astype(f32)
    scale = lax.rsqrt(jnp.mean(floats * floats, axis=-1, keepdims=True) + eps)
    normed = (floats * scale * gain_ref[...]).astype(bf16)
    out_ref[...] = (dot(place_low, normed[:, :half]) + dot(place_high, normed[:, half:])).astype(bf16)
    ids = iota((experts, rows), 0)
    shares = jnp.where(
        routes[0:1] == ids, share_ref[0:1], jnp.where(routes[1:2] == ids, share_ref[1:2], 0.0)
    ).astype(bf16)
    owner = (iota((experts, 2 * slots), 0) == iota((experts, 2 * slots), 1) // 8).astype(bf16)
    column = iota((rows, 2 * slots), 1)
    chosen = turned(codes, owner) == (column % SLOTS).astype(f32)
    picked = jnp.where(chosen, turned(shares, owner), 0.0)
    upper = (column // SLOTS) % 2 == 1
    mix_ref[0] = jnp.where(upper, 0.0, picked).astype(bf16)
    mix_ref[1] = jnp.where(upper, picked, 0.0).astype(bf16)
    for copy in large:
        copy.wait()


def prep(tokens, gain, routes, lengths, shares, w_gate, w_up, w_down):
    rows, width = tokens.shape
    hidden = w_gate.shape[2]
    chips = lax.axis_size("ep")
    return pl.pallas_call(
        prep_kernel,
        name="prep",
        out_shape=(
            jax.ShapeDtypeStruct((8 * chips, width // 2), bf16),
            pltpu.VMEM((2, rows, 16 * chips), bf16),
            pltpu.VMEM((2, width, hidden), bf16),
            pltpu.VMEM((hidden, width), bf16),
        ),
        in_specs=[pl.BlockSpec(memory_space=pltpu.HBM)] * 8,
        out_specs=(pl.BlockSpec(memory_space=pltpu.VMEM),) * 4,
        scratch_shapes=[
            pltpu.VMEM(tokens.shape, bf16),
            pltpu.VMEM(gain.shape, f32),
            pltpu.VMEM(routes.shape, jnp.int32),
            pltpu.VMEM(lengths.shape, jnp.int32),
            pltpu.VMEM(shares.shape, f32),
            pltpu.SemaphoreType.DMA((5,)),
            pltpu.SemaphoreType.DMA((3,)),
        ],
        compiler_params=pltpu.CompilerParams(vmem_limit_bytes=12 << 20),
    )(*in_hbm(tokens, gain, routes, lengths, shares, w_gate, w_up, w_down))


def expert_kernel(in_ref, sgu_ref, sd_ref, wg_ref, wu_ref, wd_ref, out_ref, x_buf, y_buf, h_buf):
    me = lax.axis_index("tp")
    hidden, width = sd_ref.shape
    half = width // 2
    parts = hidden // CHUNK
    blocks = width // CHUNK
    pairs = in_ref.shape[0] // 16
    slots = 8 * pairs
    arrived = in_ref[...].astype(f32).reshape(pairs, 2, 8, half)
    even, odd = arrived[:, 0], arrived[:, 1]
    low = iota((pairs, 8, half), 1) < SLOTS
    first = jnp.where(low, even, pltpu.roll(odd, SLOTS, 1)).reshape(slots, half)
    second = jnp.where(low, pltpu.roll(even, SLOTS, 1), odd).reshape(slots, half)
    peak = jnp.zeros((slots, 128), f32)
    for i in range(half // 128):
        lanes = slice(i * 128, (i + 1) * 128)
        peak = jnp.maximum(peak, jnp.maximum(jnp.abs(first[:, lanes]), jnp.abs(second[:, lanes])))
    filled = lax.dot_general(
        jnp.ones((8, 128), bf16), (peak > 0.0).astype(bf16), (((1,), (1,)), ((), ())), preferred_element_type=f32
    )
    live = filled > 0.0
    earlier = (iota((slots, slots), 0) < iota((slots, slots), 1)).astype(bf16)
    place = jnp.where(live, dot(live.astype(bf16), earlier), -1.0)
    amount = jnp.sum(live[0:1].astype(jnp.int32))
    squeeze = (iota((slots, slots), 0).astype(f32) == place[0:1]).astype(bf16)
    x_buf[:, :half] = dot(squeeze, first.astype(bf16)).astype(bf16)
    x_buf[:, half:] = dot(squeeze, second.astype(bf16)).astype(bf16)

    def hide(rows, gates, ups, base):
        x = x_buf[:rows]
        for i in range(parts):
            cols = pl.ds(i * CHUNK, CHUNK)
            gate = dot(x, gates[:, cols])
            up = dot(x, ups[:, cols])
            h_buf[:rows, pl.ds(base + i * CHUNK, CHUNK)] = (gate / (1.0 + jnp.exp(-gate)) * up).astype(bf16)

    def run(rows):
        hide(rows, sgu_ref.at[0], sgu_ref.at[1], 0)
        hide(rows, wg_ref.at[me], wu_ref.at[me], hidden)
        for i in range(blocks):
            cols = pl.ds(i * CHUNK, CHUNK)
            total = dot(h_buf[:rows, :hidden], sd_ref[:, cols]) + dot(h_buf[:rows, hidden:], wd_ref[me, :, cols])
            y_buf[:rows, cols] = total.astype(bf16)
        if rows < slots:
            y_buf[rows:] = jnp.zeros((slots - rows, width), bf16)

    few = slots * 3 // 4

    @pl.when(amount <= few)
    def _():
        run(few)

    @pl.when(amount > few)
    def _():
        run(slots)

    low = iota((pairs, 8, CHUNK), 1) < SLOTS

    def spread(i):
        return turned(squeeze, y_buf[:, i * CHUNK : (i + 1) * CHUNK]).reshape(pairs, 8, CHUNK)

    for core in range(2):
        a, b = spread(2 * core), spread(2 * core + 1)
        out_ref[:, 0, core] = jnp.where(low, a, pltpu.roll(b, SLOTS, 1)).astype(bf16)
        out_ref[:, 1, core] = jnp.where(low, pltpu.roll(a, SLOTS, 1), b).astype(bf16)


def expert(arrived, gate_up, down, w_gate, w_up, w_down):
    hidden, width = down.shape
    rows = arrived.shape[0] // 2
    vmem = pl.BlockSpec(memory_space=pltpu.VMEM)
    return pl.pallas_call(
        expert_kernel,
        name="expert",
        out_shape=jax.ShapeDtypeStruct((rows // 8, 2, 2, 8, width // 4), bf16),
        in_specs=[vmem] * 6,
        out_specs=vmem,
        scratch_shapes=[
            pltpu.VMEM((rows, width), bf16),
            pltpu.VMEM((rows, width), bf16),
            pltpu.VMEM((rows, 2 * hidden), bf16),
        ],
        compiler_params=pltpu.CompilerParams(vmem_limit_bytes=8 << 20),
    )(arrived, gate_up, down, *[pltpu.with_memory_space_constraint(w, pltpu.VMEM) for w in (w_gate, w_up, w_down)])


def combine_kernel(in_ref, mix_ref, out_ref):
    quarter = in_ref.shape[1]
    for part in range(2):
        out_ref[:, part * quarter : (part + 1) * quarter] = dot(mix_ref[part], in_ref[...]).astype(bf16)


def combine(returned, mix):
    vmem = pl.BlockSpec(memory_space=pltpu.VMEM)
    return pl.pallas_call(
        combine_kernel,
        name="combine",
        out_shape=jax.ShapeDtypeStruct((mix.shape[1], 2 * returned.shape[1]), bf16),
        in_specs=[vmem] * 2,
        out_specs=vmem,
        compiler_params=pltpu.CompilerParams(vmem_limit_bytes=8 << 20),
    )(returned, mix)


def per_device(tokens, norm_gain, routing, route_weights, lengths, w_gate, w_up, w_down):
    chips = lax.axis_size("ep")
    width = tokens.shape[1]
    routes = routing.T
    weights = route_weights.T
    spans = lengths.reshape(1, -1)
    outgoing, mix, gate_up, down = prep(
        tokens, norm_gain.reshape(1, -1), routes, spans, weights, w_gate, w_up, w_down
    )
    gate_up, down = (lax.ppermute(half, "tp", [(0, 1), (1, 0)]) for half in (gate_up, down))
    arrived = lax.all_to_all(outgoing.reshape(chips, 8, width // 2), "ep", split_axis=0, concat_axis=0, tiled=True)
    results = expert(arrived.reshape(chips * 8, width // 2), gate_up, down, w_gate, w_up, w_down)
    returned = lax.all_to_all(
        results.reshape(2 * chips, 8, width // 4), ("ep", "tp"), split_axis=0, concat_axis=0, tiled=True
    )
    return combine(returned.reshape(chips * 16, width // 4), mix)


def solution(mesh):
    placed = (
        P("ep", None),
        P(),
        P("ep", None),
        P("ep", None),
        P("ep"),
        P("ep", None, "tp"),
        P("ep", None, "tp"),
        P("ep", "tp", None),
    )
    return jax.shard_map(
        per_device, mesh=mesh, in_specs=placed, out_specs=P("ep", "tp"), check_vma=False
    )
```

```python
import jax
import jax.numpy as jnp
from jax import lax
from jax.experimental import pallas as pl
from jax.experimental.pallas import tpu as pltpu
from jax.sharding import PartitionSpec as P

SPAN = 4
SLOTS = 4
CHUNK = 256
eps = 1e-06
f32 = jnp.float32
bf16 = jnp.bfloat16


def dot(a, b):
    return jnp.dot(a, b, preferred_element_type=f32)


def turned(a, b):
    return lax.dot_general(a, b, (((0,), (0,)), ((), ())), preferred_element_type=f32)


def iota(shape, dim):
    return lax.broadcasted_iota(jnp.int32, shape, dim)


def in_hbm(*arrays):
    return [pltpu.with_memory_space_constraint(x, pltpu.HBM) for x in arrays]


def slot_codes(routes, lengths, experts):
    rows = routes.shape[1]
    seqs = lengths.shape[1]
    spread = (iota((seqs, rows), 1) // SPAN == iota((seqs, rows), 0)).astype(bf16)
    spans = dot(jnp.broadcast_to(lengths.astype(bf16), (8, seqs)), spread)[0:1]
    live = (iota((1, rows), 1) % SPAN).astype(f32) < spans
    ids = iota((experts, rows), 0)
    hit = ((routes[0:1] == ids) | (routes[1:2] == ids)) & live
    earlier = (iota((rows, rows), 0) < iota((rows, rows), 1)).astype(bf16)
    before = dot(hit.astype(bf16), earlier)
    return jnp.where(hit, before, -1.0)


def fetch(pairs, sems, priority=0):
    copies = [pltpu.make_async_copy(src, dst, sems.at[i]) for i, (src, dst) in enumerate(pairs)]
    for copy in copies:
        copy.start(priority=priority)
    return copies


def folded(hidden, width):
    rest = hidden - width
    blocks = [((pl.ds(0, width), pl.ds(0, width)), (pl.ds(0, width), pl.ds(0, width)))]
    blocks.append(((pl.ds(width, rest), pl.ds(0, rest)), (pl.ds(0, rest), pl.ds(width, rest))))
    for i in range(rest // CHUNK):
        rows = pl.ds(width + i * CHUNK, CHUNK)
        blocks.append(((rows, pl.ds(rest, CHUNK)), (pl.ds(rest, CHUNK), rows)))
    return blocks


def prep_kernel(
    tok_hbm, gain_hbm, route_hbm, len_hbm, share_hbm, wg_ref, wu_ref, wd_ref,
    out_ref, mix_ref, swap_ref,
    tok_ref, gain_ref, route_ref, len_ref, share_ref, small_sems, sems,
):
    me = lax.axis_index("tp")
    small = fetch(
        (
            (route_hbm, route_ref), (len_hbm, len_ref), (tok_hbm, tok_ref), (gain_hbm, gain_ref),
            (share_hbm, share_ref),
        ),
        small_sems,
    )
    theirs = wd_ref.at[1 - me]
    folds = [(theirs.at[here], swap_ref.at[2].at[there]) for here, there in folded(*theirs.shape)]
    large = fetch([(wg_ref.at[1 - me], swap_ref.at[0]), (wu_ref.at[1 - me], swap_ref.at[1])] + folds, sems, 1)
    for copy in small[:2]:
        copy.wait()
    rows, width = tok_ref.shape
    half = width // 2
    slots = out_ref.shape[0]
    experts = slots // 4
    routes = route_ref[...]
    codes = slot_codes(routes, len_ref[...], experts).astype(bf16)
    at = iota((slots, experts), 0)
    mine = (iota((slots, experts), 1) == 2 * (at // 8) + me).astype(bf16)
    wide = dot(mine, codes)
    row = iota((slots, rows), 0)
    here = wide == (row % SLOTS).astype(f32)
    upper = (row // SLOTS) % 2 == 1
    place_low = jnp.where(here & ~upper, 1.0, 0.0).astype(bf16)
    place_high = jnp.where(here & upper, 1.0, 0.0).astype(bf16)
    for copy in small[2:]:
        copy.wait()
    floats = tok_ref[...].astype(f32)
    scale = lax.rsqrt(jnp.mean(floats * floats, axis=-1, keepdims=True) + eps)
    normed = (floats * scale * gain_ref[...]).astype(bf16)
    out_ref[...] = (dot(place_low, normed[:, :half]) + dot(place_high, normed[:, half:])).astype(bf16)
    ids = iota((experts, rows), 0)
    shares = jnp.where(
        routes[0:1] == ids, share_ref[0:1], jnp.where(routes[1:2] == ids, share_ref[1:2], 0.0)
    ).astype(bf16)
    owner = (iota((experts, 2 * slots), 0) == iota((experts, 2 * slots), 1) // 8).astype(bf16)
    column = iota((rows, 2 * slots), 1)
    chosen = turned(codes, owner) == (column % SLOTS).astype(f32)
    picked = jnp.where(chosen, turned(shares, owner), 0.0)
    upper = (column // SLOTS) % 2 == 1
    mix_ref[0] = jnp.where(upper, 0.0, picked).astype(bf16)
    mix_ref[1] = jnp.where(upper, picked, 0.0).astype(bf16)
    for copy in large:
        copy.wait()


def prep(tokens, gain, routes, lengths, shares, w_gate, w_up, w_down):
    rows, width = tokens.shape
    hidden = w_gate.shape[2]
    chips = lax.axis_size("ep")
    return pl.pallas_call(
        prep_kernel,
        name="prep",
        out_shape=(
            jax.ShapeDtypeStruct((8 * chips, width // 2), bf16),
            pltpu.VMEM((2, rows, 16 * chips), bf16),
            pltpu.VMEM((3, width, hidden), bf16),
        ),
        in_specs=[pl.BlockSpec(memory_space=pltpu.HBM)] * 8,
        out_specs=(pl.BlockSpec(memory_space=pltpu.VMEM),) * 3,
        scratch_shapes=[
            pltpu.VMEM(tokens.shape, bf16),
            pltpu.VMEM(gain.shape, f32),
            pltpu.VMEM(routes.shape, jnp.int32),
            pltpu.VMEM(lengths.shape, jnp.int32),
            pltpu.VMEM(shares.shape, f32),
            pltpu.SemaphoreType.DMA((5,)),
            pltpu.SemaphoreType.DMA((2 + len(folded(hidden, width)),)),
        ],
        compiler_params=pltpu.CompilerParams(vmem_limit_bytes=12 << 20),
    )(*in_hbm(tokens, gain, routes, lengths, shares, w_gate, w_up, w_down))


def expert_kernel(in_ref, swap_ref, wg_ref, wu_ref, wd_ref, out_ref, x_buf, y_buf, h_buf):
    me = lax.axis_index("tp")
    _, width, hidden = swap_ref.shape
    rest = hidden - width
    half = width // 2
    parts = hidden // CHUNK
    blocks = width // CHUNK
    pairs = in_ref.shape[0] // 16
    slots = 8 * pairs
    arrived = in_ref[...].astype(f32).reshape(pairs, 2, 8, half)
    even, odd = arrived[:, 0], arrived[:, 1]
    low = iota((pairs, 8, half), 1) < SLOTS
    first = jnp.where(low, even, pltpu.roll(odd, SLOTS, 1)).reshape(slots, half)
    second = jnp.where(low, pltpu.roll(even, SLOTS, 1), odd).reshape(slots, half)
    peak = jnp.zeros((slots, 128), f32)
    for i in range(half // 128):
        lanes = slice(i * 128, (i + 1) * 128)
        peak = jnp.maximum(peak, jnp.maximum(jnp.abs(first[:, lanes]), jnp.abs(second[:, lanes])))
    filled = lax.dot_general(
        jnp.ones((8, 128), bf16), (peak > 0.0).astype(bf16), (((1,), (1,)), ((), ())), preferred_element_type=f32
    )
    live = filled > 0.0
    earlier = (iota((slots, slots), 0) < iota((slots, slots), 1)).astype(bf16)
    place = jnp.where(live, dot(live.astype(bf16), earlier), -1.0)
    amount = jnp.sum(live[0:1].astype(jnp.int32))
    squeeze = (iota((slots, slots), 0).astype(f32) == place[0:1]).astype(bf16)
    x_buf[:, :half] = dot(squeeze, first.astype(bf16)).astype(bf16)
    x_buf[:, half:] = dot(squeeze, second.astype(bf16)).astype(bf16)

    def hide(rows, gates, ups, base):
        x = x_buf[:rows]
        for i in range(parts):
            cols = pl.ds(i * CHUNK, CHUNK)
            gate = dot(x, gates[:, cols])
            up = dot(x, ups[:, cols])
            h_buf[:rows, pl.ds(base + i * CHUNK, CHUNK)] = (gate / (1.0 + jnp.exp(-gate)) * up).astype(bf16)

    def run(rows):
        hide(rows, swap_ref.at[0], swap_ref.at[1], 0)
        hide(rows, wg_ref.at[me], wu_ref.at[me], hidden)
        for i in range(blocks):
            cols = pl.ds(i * CHUNK, CHUNK)
            total = dot(h_buf[:rows, hidden:], wd_ref[me, :, cols])
            total = total + dot(h_buf[:rows, :width], swap_ref[2, :, cols])
            if i * CHUNK < rest:
                total = total + dot(h_buf[:rows, width:hidden], swap_ref[2, :rest, pl.ds(width + i * CHUNK, CHUNK)])
            else:
                for j in range(rest // CHUNK):
                    part = pl.ds(width + j * CHUNK, CHUNK)
                    total = total + dot(h_buf[:rows, part], swap_ref[2, rest:, part])
            y_buf[:rows, cols] = total.astype(bf16)
        if rows < slots:
            y_buf[rows:] = jnp.zeros((slots - rows, width), bf16)

    few = slots * 3 // 4

    @pl.when(amount <= few)
    def _():
        run(few)

    @pl.when(amount > few)
    def _():
        run(slots)

    low = iota((pairs, 8, CHUNK), 1) < SLOTS

    def spread(i):
        return turned(squeeze, y_buf[:, i * CHUNK : (i + 1) * CHUNK]).reshape(pairs, 8, CHUNK)

    for core in range(2):
        a, b = spread(2 * core), spread(2 * core + 1)
        out_ref[:, 0, core] = jnp.where(low, a, pltpu.roll(b, SLOTS, 1)).astype(bf16)
        out_ref[:, 1, core] = jnp.where(low, pltpu.roll(a, SLOTS, 1), b).astype(bf16)


def expert(arrived, swapped, w_gate, w_up, w_down):
    _, width, hidden = swapped.shape
    rows = arrived.shape[0] // 2
    vmem = pl.BlockSpec(memory_space=pltpu.VMEM)
    return pl.pallas_call(
        expert_kernel,
        name="expert",
        out_shape=jax.ShapeDtypeStruct((rows // 8, 2, 2, 8, width // 4), bf16),
        in_specs=[vmem] * 5,
        out_specs=vmem,
        scratch_shapes=[
            pltpu.VMEM((rows, width), bf16),
            pltpu.VMEM((rows, width), bf16),
            pltpu.VMEM((rows, 2 * hidden), bf16),
        ],
        compiler_params=pltpu.CompilerParams(vmem_limit_bytes=8 << 20),
    )(arrived, swapped, *[pltpu.with_memory_space_constraint(w, pltpu.VMEM) for w in (w_gate, w_up, w_down)])


def combine_kernel(in_ref, mix_ref, out_ref):
    quarter = in_ref.shape[1]
    for part in range(2):
        out_ref[:, part * quarter : (part + 1) * quarter] = dot(mix_ref[part], in_ref[...]).astype(bf16)


def combine(returned, mix):
    vmem = pl.BlockSpec(memory_space=pltpu.VMEM)
    return pl.pallas_call(
        combine_kernel,
        name="combine",
        out_shape=jax.ShapeDtypeStruct((mix.shape[1], 2 * returned.shape[1]), bf16),
        in_specs=[vmem] * 2,
        out_specs=vmem,
        compiler_params=pltpu.CompilerParams(vmem_limit_bytes=8 << 20),
    )(returned, mix)


def per_device(tokens, norm_gain, routing, route_weights, lengths, w_gate, w_up, w_down):
    chips = lax.axis_size("ep")
    width = tokens.shape[1]
    routes = routing.T
    weights = route_weights.T
    spans = lengths.reshape(1, -1)
    outgoing, mix, others = prep(
        tokens, norm_gain.reshape(1, -1), routes, spans, weights, w_gate, w_up, w_down
    )
    swapped = lax.ppermute(others, "tp", [(0, 1), (1, 0)])
    arrived = lax.all_to_all(outgoing.reshape(chips, 8, width // 2), "ep", split_axis=0, concat_axis=0, tiled=True)
    results = expert(arrived.reshape(chips * 8, width // 2), swapped, w_gate, w_up, w_down)
    returned = lax.all_to_all(
        results.reshape(2 * chips, 8, width // 4), ("ep", "tp"), split_axis=0, concat_axis=0, tiled=True
    )
    return combine(returned.reshape(chips * 16, width // 4), mix)


def solution(mesh):
    placed = (
        P("ep", None),
        P(),
        P("ep", None),
        P("ep", None),
        P("ep"),
        P("ep", None, "tp"),
        P("ep", None, "tp"),
        P("ep", "tp", None),
    )
    return jax.shard_map(
        per_device, mesh=mesh, in_specs=placed, out_specs=P("ep", "tp"), check_vma=False
    )
```

```python
import jax
import jax.numpy as jnp
from jax import lax
from jax.experimental import pallas as pl
from jax.experimental.pallas import tpu as pltpu
from jax.sharding import PartitionSpec as P

SPAN = 4
SLOTS = 4
CHUNK = 256
eps = 1e-06
f32 = jnp.float32
bf16 = jnp.bfloat16


def dot(a, b):
    return jnp.dot(a, b, preferred_element_type=f32)


def turned(a, b):
    return lax.dot_general(a, b, (((0,), (0,)), ((), ())), preferred_element_type=f32)


def iota(shape, dim):
    return lax.broadcasted_iota(jnp.int32, shape, dim)


def in_hbm(*arrays):
    return [pltpu.with_memory_space_constraint(x, pltpu.HBM) for x in arrays]


def slot_codes(routes, lengths, experts):
    rows = routes.shape[1]
    seqs = lengths.shape[1]
    spread = (iota((seqs, rows), 1) // SPAN == iota((seqs, rows), 0)).astype(bf16)
    spans = dot(jnp.broadcast_to(lengths.astype(bf16), (8, seqs)), spread)[0:1]
    live = (iota((1, rows), 1) % SPAN).astype(f32) < spans
    ids = iota((experts, rows), 0)
    hit = ((routes[0:1] == ids) | (routes[1:2] == ids)) & live
    earlier = (iota((rows, rows), 0) < iota((rows, rows), 1)).astype(bf16)
    before = dot(hit.astype(bf16), earlier)
    return jnp.where(hit, before, -1.0)


def fetch(pairs, sems, priority=0):
    copies = [pltpu.make_async_copy(src, dst, sems.at[i]) for i, (src, dst) in enumerate(pairs)]
    for copy in copies:
        copy.start(priority=priority)
    return copies


def folded(hidden, width):
    rest = hidden - width
    blocks = [((pl.ds(0, width), pl.ds(0, width)), (pl.ds(0, width), pl.ds(0, width)))]
    blocks.append(((pl.ds(width, rest), pl.ds(0, rest)), (pl.ds(0, rest), pl.ds(width, rest))))
    for i in range(rest // CHUNK):
        rows = pl.ds(width + i * CHUNK, CHUNK)
        blocks.append(((rows, pl.ds(rest, CHUNK)), (pl.ds(rest, CHUNK), rows)))
    return blocks


def prep_kernel(
    tok_hbm, gain_hbm, route_hbm, len_hbm, share_hbm, wg_ref, wu_ref, wd_ref,
    out_ref, mix_ref, swap_ref,
    tok_ref, gain_ref, route_ref, len_ref, share_ref, small_sems, sems,
):
    me = lax.axis_index("tp")
    small = fetch(
        (
            (route_hbm, route_ref), (len_hbm, len_ref), (tok_hbm, tok_ref), (gain_hbm, gain_ref),
            (share_hbm, share_ref),
        ),
        small_sems,
    )
    theirs = wd_ref.at[1 - me]
    folds = [(theirs.at[here], swap_ref.at[2].at[there]) for here, there in folded(*theirs.shape)]
    large = fetch([(wg_ref.at[1 - me], swap_ref.at[0]), (wu_ref.at[1 - me], swap_ref.at[1])] + folds, sems, 1)
    for copy in small[:2]:
        copy.wait()
    rows, width = tok_ref.shape
    half = width // 2
    slots = out_ref.shape[0]
    experts = slots // 4
    routes = route_ref[...]
    codes = slot_codes(routes, len_ref[...], experts).astype(bf16)
    at = iota((slots, experts), 0)
    mine = (iota((slots, experts), 1) == 2 * (at // 8) + me).astype(bf16)
    wide = dot(mine, codes)
    row = iota((slots, rows), 0)
    here = wide == (row % SLOTS).astype(f32)
    upper = (row // SLOTS) % 2 == 1
    place_low = jnp.where(here & ~upper, 1.0, 0.0).astype(bf16)
    place_high = jnp.where(here & upper, 1.0, 0.0).astype(bf16)
    for copy in small[2:]:
        copy.wait()
    floats = tok_ref[...].astype(f32)
    scale = lax.rsqrt(jnp.mean(floats * floats, axis=-1, keepdims=True) + eps)
    normed = (floats * scale * gain_ref[...]).astype(bf16)
    out_ref[...] = (dot(place_low, normed[:, :half]) + dot(place_high, normed[:, half:])).astype(bf16)
    ids = iota((experts, rows), 0)
    shares = jnp.where(
        routes[0:1] == ids, share_ref[0:1], jnp.where(routes[1:2] == ids, share_ref[1:2], 0.0)
    ).astype(bf16)
    owner = (iota((experts, 2 * slots), 0) == iota((experts, 2 * slots), 1) // 8).astype(bf16)
    column = iota((rows, 2 * slots), 1)
    chosen = turned(codes, owner) == (column % SLOTS).astype(f32)
    picked = jnp.where(chosen, turned(shares, owner), 0.0)
    upper = (column // SLOTS) % 2 == 1
    mix_ref[0] = jnp.where(upper, 0.0, picked).astype(bf16)
    mix_ref[1] = jnp.where(upper, picked, 0.0).astype(bf16)
    for copy in large:
        copy.wait()


def prep(tokens, gain, routes, lengths, shares, w_gate, w_up, w_down):
    rows, width = tokens.shape
    hidden = w_gate.shape[2]
    chips = lax.axis_size("ep")
    return pl.pallas_call(
        prep_kernel,
        name="prep",
        out_shape=(
            jax.ShapeDtypeStruct((8 * chips, width // 2), bf16),
            pltpu.VMEM((2, rows, 16 * chips), bf16),
            pltpu.VMEM((3, width, hidden), bf16),
        ),
        in_specs=[pl.BlockSpec(memory_space=pltpu.HBM)] * 8,
        out_specs=(pl.BlockSpec(memory_space=pltpu.VMEM),) * 3,
        scratch_shapes=[
            pltpu.VMEM(tokens.shape, bf16),
            pltpu.VMEM(gain.shape, f32),
            pltpu.VMEM(routes.shape, jnp.int32),
            pltpu.VMEM(lengths.shape, jnp.int32),
            pltpu.VMEM(shares.shape, f32),
            pltpu.SemaphoreType.DMA((5,)),
            pltpu.SemaphoreType.DMA((2 + len(folded(hidden, width)),)),
        ],
        compiler_params=pltpu.CompilerParams(vmem_limit_bytes=12 << 20),
    )(*in_hbm(tokens, gain, routes, lengths, shares, w_gate, w_up, w_down))


def expert_kernel(in_ref, swap_ref, wg_ref, wu_ref, wd_ref, out_ref, x_buf, y_buf, h_buf):
    me = lax.axis_index("tp")
    _, width, hidden = swap_ref.shape
    rest = hidden - width
    half = width // 2
    parts = hidden // CHUNK
    blocks = width // CHUNK
    pairs = in_ref.shape[0] // 16
    slots = 8 * pairs
    low = iota((pairs, 8, 128), 1) < SLOTS
    peak = jnp.zeros((pairs, 8, 128), f32)
    for i in range(half // 128):
        arrived = in_ref[:, i * 128 : (i + 1) * 128].astype(f32).reshape(pairs, 2, 8, 128)
        even, odd = arrived[:, 0], arrived[:, 1]
        first = jnp.where(low, even, pltpu.roll(odd, SLOTS, 1))
        second = jnp.where(low, pltpu.roll(even, SLOTS, 1), odd)
        y_buf[:, i * 128 : (i + 1) * 128] = first.reshape(slots, 128).astype(bf16)
        y_buf[:, half + i * 128 : half + (i + 1) * 128] = second.reshape(slots, 128).astype(bf16)
        peak = jnp.maximum(peak, jnp.maximum(jnp.abs(first), jnp.abs(second)))
    peak = peak.reshape(slots, 128)
    filled = lax.dot_general(
        jnp.ones((8, 128), bf16), (peak > 0.0).astype(bf16), (((1,), (1,)), ((), ())), preferred_element_type=f32
    )
    live = filled > 0.0
    earlier = (iota((slots, slots), 0) < iota((slots, slots), 1)).astype(bf16)
    place = jnp.where(live, dot(live.astype(bf16), earlier), -1.0)
    amount = jnp.sum(live[0:1].astype(jnp.int32))
    squeeze = (iota((slots, slots), 0).astype(f32) == place[0:1]).astype(bf16)
    for i in range(blocks):
        cols = slice(i * CHUNK, (i + 1) * CHUNK)
        x_buf[:, cols] = dot(squeeze, y_buf[:, cols]).astype(bf16)

    def hide(rows, gates, ups, base):
        x = x_buf[:rows]
        for i in range(parts):
            cols = pl.ds(i * CHUNK, CHUNK)
            gate = dot(x, gates[:, cols])
            up = dot(x, ups[:, cols])
            h_buf[:rows, pl.ds(base + i * CHUNK, CHUNK)] = (gate / (1.0 + jnp.exp(-gate)) * up).astype(bf16)

    def run(rows):
        hide(rows, swap_ref.at[0], swap_ref.at[1], 0)
        hide(rows, wg_ref.at[me], wu_ref.at[me], hidden)
        for i in range(blocks):
            cols = pl.ds(i * CHUNK, CHUNK)
            total = dot(h_buf[:rows, hidden:], wd_ref[me, :, cols])
            total = total + dot(h_buf[:rows, :width], swap_ref[2, :, cols])
            if i * CHUNK < rest:
                total = total + dot(h_buf[:rows, width:hidden], swap_ref[2, :rest, pl.ds(width + i * CHUNK, CHUNK)])
            else:
                for j in range(rest // CHUNK):
                    part = pl.ds(width + j * CHUNK, CHUNK)
                    total = total + dot(h_buf[:rows, part], swap_ref[2, rest:, part])
            y_buf[:rows, cols] = total.astype(bf16)
        if rows < slots:
            y_buf[rows:] = jnp.zeros((slots - rows, width), bf16)

    few = slots * 3 // 4

    @pl.when(amount <= few)
    def _():
        run(few)

    @pl.when(amount > few)
    def _():
        run(slots)

    low = iota((pairs, 8, CHUNK), 1) < SLOTS

    def spread(i):
        return turned(squeeze, y_buf[:, i * CHUNK : (i + 1) * CHUNK]).reshape(pairs, 8, CHUNK)

    for core in range(2):
        a, b = spread(2 * core), spread(2 * core + 1)
        out_ref[:, 0, core] = jnp.where(low, a, pltpu.roll(b, SLOTS, 1)).astype(bf16)
        out_ref[:, 1, core] = jnp.where(low, pltpu.roll(a, SLOTS, 1), b).astype(bf16)


def expert(arrived, swapped, w_gate, w_up, w_down):
    _, width, hidden = swapped.shape
    rows = arrived.shape[0] // 2
    vmem = pl.BlockSpec(memory_space=pltpu.VMEM)
    return pl.pallas_call(
        expert_kernel,
        name="expert",
        out_shape=jax.ShapeDtypeStruct((rows // 8, 2, 2, 8, width // 4), bf16),
        in_specs=[vmem] * 5,
        out_specs=vmem,
        scratch_shapes=[
            pltpu.VMEM((rows, width), bf16),
            pltpu.VMEM((rows, width), bf16),
            pltpu.VMEM((rows, 2 * hidden), bf16),
        ],
        compiler_params=pltpu.CompilerParams(vmem_limit_bytes=8 << 20),
    )(arrived, swapped, *[pltpu.with_memory_space_constraint(w, pltpu.VMEM) for w in (w_gate, w_up, w_down)])


def combine_kernel(in_ref, mix_ref, out_ref):
    quarter = in_ref.shape[1]
    for part in range(2):
        out_ref[:, part * quarter : (part + 1) * quarter] = dot(mix_ref[part], in_ref[...]).astype(bf16)


def combine(returned, mix):
    vmem = pl.BlockSpec(memory_space=pltpu.VMEM)
    return pl.pallas_call(
        combine_kernel,
        name="combine",
        out_shape=jax.ShapeDtypeStruct((mix.shape[1], 2 * returned.shape[1]), bf16),
        in_specs=[vmem] * 2,
        out_specs=vmem,
        compiler_params=pltpu.CompilerParams(vmem_limit_bytes=8 << 20),
    )(returned, mix)


def per_device(tokens, norm_gain, routing, route_weights, lengths, w_gate, w_up, w_down):
    chips = lax.axis_size("ep")
    width = tokens.shape[1]
    routes = routing.T
    weights = route_weights.T
    spans = lengths.reshape(1, -1)
    outgoing, mix, others = prep(
        tokens, norm_gain.reshape(1, -1), routes, spans, weights, w_gate, w_up, w_down
    )
    swapped = lax.ppermute(others, "tp", [(0, 1), (1, 0)])
    arrived = lax.all_to_all(outgoing.reshape(chips, 8, width // 2), "ep", split_axis=0, concat_axis=0, tiled=True)
    results = expert(arrived.reshape(chips * 8, width // 2), swapped, w_gate, w_up, w_down)
    returned = lax.all_to_all(
        results.reshape(2 * chips, 8, width // 4), ("ep", "tp"), split_axis=0, concat_axis=0, tiled=True
    )
    return combine(returned.reshape(chips * 16, width // 4), mix)


def solution(mesh):
    placed = (
        P("ep", None),
        P(),
        P("ep", None),
        P("ep", None),
        P("ep"),
        P("ep", None, "tp"),
        P("ep", None, "tp"),
        P("ep", "tp", None),
    )
    return jax.shard_map(
        per_device, mesh=mesh, in_specs=placed, out_specs=P("ep", "tp"), check_vma=False
    )
```
